256 devices in a mesh: sp: 64 (over z, x, core), tp: 4 (over y).
Axes of the slice: x: 4, y: 4, z: 8, core: 2. Of those that a mesh axis runs over, the one named last changes fastest.
Arguments:
- inputs: bfloat16 [40960, 2048], P('sp', 'tp'), may hold values from -6 to 6
- norm_gain: bfloat16 [2048], P('tp'), may hold values from 0.099609375 to 1.8984375
- query_weight: bfloat16 [2048, 2048], P('sp', 'tp'), may hold values from -0.125 to 0.125
- key_weight: bfloat16 [2048, 2048], P('sp', 'tp'), may hold values from -0.125 to 0.125
- value_weight: bfloat16 [2048, 2048], P('sp', 'tp'), may hold values from -0.125 to 0.125
- outgate_weight: bfloat16 [2048, 2048], P('sp', 'tp'), may hold values from -0.125 to 0.125
- inputgate_weight: bfloat16 [2048, 8], replicated, may hold values from -1 to 1
- forget_weight: bfloat16 [2048, 8], replicated, may hold values from -0.125 to 0.125
- forget_bias: float32 [8], P('tp'), may hold values from -1.1 to 2.25
- conv_query: float32 [4, 2048], P(None, 'tp'), may hold values from -3 to 3
- conv_key: float32 [4, 2048], P(None, 'tp'), may hold values from -3 to 3
- cell_gain: float32 [2048], P('tp'), may hold values from 0.1 to 1.9
- pool_weight: bfloat16 [2048, 1024], P('sp', 'tp'), may hold values from -0.125 to 0.125
- group_weight: bfloat16 [8, 128, 128], P('tp'), may hold values from -0.5 to 0.5
- pool_gain: float32 [1024], P('tp'), may hold values from 0.1 to 1.9
- cell_out_weight: bfloat16 [2048, 2048], P('tp', 'sp'), may hold values from -0.109375 to 0.109375
- pool_out_weight: bfloat16 [1024, 2048], P('tp', 'sp'), may hold values from -0.109375 to 0.109375
Outputs:
- mixed: bfloat16 [40960, 2048], P(('sp', 'tp'))
The draws below stay inside these ranges and needn't reach their ends.
All inputs are finite; a program needn't handle non-finite values.
Results may differ from the reference program's by a relative error of at most 0.013.
The reference program's roundings to bfloat16 on the way (of `normed`, `cell_mix`, `pooled` and `pool_mix`) count: a program that leaves them out, or rounds other values in their place, can miss the bound.
Values may be sent and summed in bfloat16 or wider, within the bound.
A program may use at most 128 MiB of HBM per device.

```python
import math
import jax
import jax.numpy as jnp
from jax import lax

D = 2048
HM = 8
DH = 256
PG = 8
CG = 128
LEVELS = 4
CONV = 4
TOK_DEV = 640
TOKENS = 40960
N_SP = 64


def draw_inputs(key, part):
    jitter = jax.random.normal(jax.random.fold_in(key, 12), (TOKENS, D), jnp.float32)
    values = jnp.clip(jitter, -6.0, 6.0)
    return values.astype(jnp.bfloat16)


def draw_inputgate_weight(key, part):
    spread = D ** (-0.5)
    jitter = jnp.clip(jax.random.normal(jax.random.fold_in(key, 13), (D, HM), jnp.float32), -6.0, 6.0) * spread
    values = jitter
    return values.astype(jnp.bfloat16)


def block_scale(own_key, shape, cuts, smallest, top_value):
    def one(dim, blocks):
        draws = jax.random.uniform(jax.random.fold_in(jax.random.fold_in(own_key, 6), dim), (blocks,), jnp.float32, smallest / len(cuts), top_value / len(cuts))
        return jnp.repeat(jnp.exp(draws), shape[dim] // blocks).reshape((-1,) + (1,) * (len(shape) - dim - 1))

    gain = one(*cuts[0])
    for cut in cuts[1:]:
        gain = gain * one(*cut)
    return gain


def normal_values(key, extent, width, most, split=(), kind=jnp.bfloat16):
    values = jax.random.normal(key, extent, jnp.float32) * width
    if len(split) > 0:
        values = block_scale(key, extent, split, -0.22, 0.18) * values
    return jnp.clip(values, min=-most, max=most).astype(kind)


def setup_inputs(seed: int = 0) -> dict:
    key_of = jax.random.split(jax.random.key(seed), 18)
    return {
        "inputs": draw_inputs(jax.random.fold_in(key_of[17], 71), 0),
        "norm_gain": jnp.clip(1.0 + 0.18 * jax.random.normal(key_of[1], (D,), jnp.float32), 0.099609375, 1.8984375).astype(jnp.bfloat16),
        "query_weight": normal_values(key_of[2], (D, HM * DH), D ** -0.5, 0.125, ((0, 64), (1, 4))),
        "key_weight": normal_values(key_of[3], (D, HM * DH), D ** -0.5, 0.125, ((0, 64), (1, 4))),
        "value_weight": normal_values(key_of[4], (D, HM * DH), D ** -0.5, 0.125, ((0, 64), (1, 4))),
        "outgate_weight": normal_values(key_of[5], (D, HM * DH), D ** -0.5, 0.125, ((0, 64), (1, 4))),
        "inputgate_weight": draw_inputgate_weight(jax.random.fold_in(key_of[17], 71), 0),
        "forget_weight": normal_values(key_of[7], (D, HM), D ** -0.5, 0.125),
        "forget_bias": jnp.clip(-1.1 + 3.35 * jax.random.uniform(key_of[8], (HM,), jnp.float32) ** block_scale(key_of[8], (HM,), ((0, 4),), -0.2, 0.2), -1.1, 2.25),
        "conv_query": normal_values(key_of[9], (CONV, HM * DH), CONV ** -0.5, 3.0, ((1, 4),), jnp.float32),
        "conv_key": normal_values(key_of[10], (CONV, HM * DH), CONV ** -0.5, 3.0, ((1, 4),), jnp.float32),
        "cell_gain": jnp.clip(1.0 + 0.18 * jax.random.normal(key_of[11], (HM * DH,), jnp.float32), 0.1, 1.9),
        "pool_weight": normal_values(key_of[12], (D, PG * CG), D ** -0.5, 0.125, ((0, 64), (1, 4))),
        "group_weight": normal_values(key_of[13], (PG, CG, CG), CG ** -0.5, 0.5, ((0, 4),)),
        "pool_gain": jnp.clip(1.0 + 0.18 * jax.random.normal(key_of[14], (PG * CG,), jnp.float32), 0.1, 1.9),
        "cell_out_weight": normal_values(key_of[15], (HM * DH, D), (HM * DH + PG * CG) ** -0.5, 0.109375, ((0, 4), (1, 64))),
        "pool_out_weight": normal_values(key_of[16], (PG * CG, D), (HM * DH + PG * CG) ** -0.5, 0.109375, ((0, 4), (1, 64))),
    }


epsilon = 1e-06
big_negative = -1e+30
highest = lax.Precision.HIGHEST

def causal_taps(padded, taps):
    span_rows = padded.shape[0] - taps.shape[0] + 1
    running = jnp.zeros((span_rows, padded.shape[1]), jnp.float32)
    for lag_index in range(taps.shape[0]):
        running = running + taps[lag_index] * padded[lag_index:lag_index + span_rows].astype(jnp.float32)
    return running

def cell_block(carry, block_inputs):
    memory, normalizer, stabilizer = carry
    queries, key_rows, value_rows, log_in, log_keep = block_inputs
    query_wide = queries.astype(jnp.float32)
    key_wide = key_rows.astype(jnp.float32)
    value_wide = value_rows.astype(jnp.float32)
    length = queries.shape[0]
    cumulative = jnp.cumsum(log_keep, axis=0)
    cum_heads = cumulative.T
    in_heads = log_in.T
    causal = jnp.arange(length)[:, None] >= jnp.arange(length)[None, :]
    decay_log = cum_heads[:, :, None] - cum_heads[:, None, :] + in_heads[:, None, :]
    decay_log = jnp.where(causal[None, :, :], decay_log, -jnp.inf)
    carried_log = cum_heads + stabilizer[:, None]
    ceiling = jnp.maximum(carried_log, lax.optimization_barrier(jnp.max(decay_log, axis=2)))
    within = jnp.exp(decay_log - ceiling[:, :, None])
    carried = jnp.exp(carried_log - ceiling)
    raw_scores = jnp.einsum('thd,shd->hts', query_wide, key_wide, precision=highest)
    scores = (raw_scores * within).astype(jnp.bfloat16).astype(jnp.float32)
    numerator = carried.T[:, :, None] * jnp.einsum('hvk,thk->thv', memory, query_wide, precision=highest)
    numerator = numerator + jnp.einsum('hts,shv->thv', scores, value_wide, precision=highest)
    denominator = carried.T * jnp.einsum('hk,thk->th', normalizer, query_wide, precision=highest) + lax.optimization_barrier(jnp.sum(scores, axis=2)).T
    hidden = numerator / jnp.maximum(jnp.abs(denominator), jnp.exp(-ceiling.T))[:, :, None]
    final_log = cumulative[-1]
    lead_log = final_log[None, :] - cumulative + log_in
    new_stab = jnp.maximum(final_log + stabilizer, lax.optimization_barrier(jnp.max(lead_log, axis=0)))
    share_weight = jnp.exp(lead_log - new_stab[None, :])
    fade_factor = jnp.exp(final_log + stabilizer - new_stab)
    weighted = (value_wide * share_weight[:, :, None]).astype(jnp.bfloat16).astype(jnp.float32)
    memory = fade_factor[:, None, None] * memory + jnp.einsum('shv,shk->hvk', weighted, key_wide, precision=highest)
    normalizer = fade_factor[:, None] * normalizer + jnp.einsum('sh,shk->hk', share_weight, key_wide, precision=highest)
    return ((memory, normalizer, new_stab), hidden)

def reference(inputs, norm_gain, query_weight, key_weight, value_weight, outgate_weight, inputgate_weight, forget_weight, forget_bias, conv_query, conv_key, cell_gain, pool_weight, group_weight, pool_gain, cell_out_weight, pool_out_weight):
    wide_in = inputs.astype(jnp.float32)
    inverse_rms = lax.rsqrt(lax.optimization_barrier(jnp.mean(wide_in * wide_in, axis=1, keepdims=True)) + epsilon)
    normed = (wide_in * norm_gain.astype(jnp.float32)).astype(jnp.bfloat16)

    def project(weight):
        return jnp.dot(normed, weight, preferred_element_type=jnp.float32) * inverse_rms
    query_pre = project(query_weight).astype(jnp.bfloat16)
    key_pre = project(key_weight).astype(jnp.bfloat16)
    value_rows = project(value_weight).astype(jnp.bfloat16)
    outgate_pre = project(outgate_weight).astype(jnp.bfloat16)
    pool_pre = project(pool_weight).astype(jnp.bfloat16)
    log_in = project(inputgate_weight)
    log_keep = jax.nn.log_sigmoid(project(forget_weight) + forget_bias + math.log(TOKENS))
    margin = conv_query.shape[0] - 1
    query_taps = causal_taps(jnp.pad(query_pre, ((margin, 0), (0, 0))), conv_query)
    key_taps = causal_taps(jnp.pad(key_pre, ((margin, 0), (0, 0))), conv_key)
    queries = (jax.nn.silu(query_taps) * DH ** (-0.5)).astype(jnp.bfloat16)
    key_rows = jax.nn.silu(key_taps).astype(jnp.bfloat16)

    def to_blocks(array):
        return array.reshape((N_SP, TOK_DEV) + array.shape[1:])

    def split_heads(array):
        return array.reshape(TOKENS, HM, DH)
    start_carry = (jnp.zeros((HM, DH, DH), jnp.float32), jnp.zeros((HM, DH), jnp.float32), jnp.full((HM,), big_negative, jnp.float32))
    block_inputs = (to_blocks(split_heads(queries)), to_blocks(split_heads(key_rows)), to_blocks(split_heads(value_rows)), to_blocks(log_in), to_blocks(log_keep))
    ignored, hidden = lax.scan(cell_block, start_carry, block_inputs)
    hidden = hidden.reshape(TOKENS, HM, DH)
    normalized = hidden * lax.rsqrt(lax.optimization_barrier(jnp.mean(hidden * hidden, axis=2, keepdims=True)) + epsilon)
    cell_mix = (normalized.reshape(TOKENS, HM * DH) * cell_gain * jax.nn.sigmoid(outgate_pre.astype(jnp.float32))).astype(jnp.bfloat16)
    widest = 2 ** LEVELS - 1
    padded_pool = jnp.pad(pool_pre, ((widest, 0), (0, 0))).astype(jnp.float32)
    position = jnp.arange(TOKENS)
    pieces = []
    for group_index in range(PG):
        reach_rows = 2 ** (1 + group_index % LEVELS)
        columns = padded_pool[:, group_index * CG:(group_index + 1) * CG]
        window_sum = jnp.zeros((TOKENS, CG), jnp.float32)
        for lag_index in range(reach_rows):
            window_sum = window_sum + columns[widest - lag_index:widest - lag_index + TOKENS]
        counted = jnp.minimum(position + 1, reach_rows).astype(jnp.float32)[:, None]
        pieces.append(window_sum / counted - columns[widest:])
    pooled = jnp.stack(pieces, axis=1).astype(jnp.bfloat16)
    grouped_out = jnp.einsum('sgc,gcd->sgd', pooled.astype(jnp.float32), group_weight.astype(jnp.float32), precision=highest)
    pool_mix = (grouped_out.reshape(TOKENS, PG * CG) * pool_gain).astype(jnp.bfloat16)
    mixed = jnp.dot(cell_mix, cell_out_weight, preferred_element_type=jnp.float32)
    mixed = mixed + jnp.dot(pool_mix, pool_out_weight, preferred_element_type=jnp.float32)
    return mixed.astype(jnp.bfloat16)
```

```python
import functools
import math

import jax
import jax.numpy as jnp
from jax import lax
from jax.experimental import pallas as pl
from jax.experimental.pallas import tpu as pltpu
from jax.sharding import Mesh
from jax.sharding import PartitionSpec as P

LEVELS = 4
NZ, NX, NC, NT = 8, 4, 2, 4
TOK = 640
HALO = 32
ROWS = TOK + HALO
SP = ("z", "x", "c")
SP_TP = ("z", "x", "c", "tp")
MESH = pl.DeviceIdType.MESH
epsilon = 1e-06
big_negative = -1e30
f32 = jnp.float32
bf16 = jnp.bfloat16


class Ring:
    def __init__(self, send_sems, recv_sems, local_sems):
        self.send_sems, self.recv_sems, self.local_sems = send_sems, recv_sems, local_sems
        self.used = 0
        self.used_local = 0
        self.pending = []

    def copy(self, src, dst, **where):
        k = self.used
        self.used += 1
        c = pltpu.make_async_remote_copy(
            src_ref=src,
            dst_ref=dst,
            send_sem=self.send_sems.at[k],
            recv_sem=self.recv_sems.at[k],
            device_id=where,
            device_id_type=MESH,
        )
        c.start()
        self.pending.append(c)
        return c

    def local(self, src, dst):
        k = self.used_local
        self.used_local += 1
        c = pltpu.make_async_copy(src, dst, self.local_sems.at[k])
        c.start()
        return c

    def drain(self):
        for c in self.pending:
            c.wait_send()
        self.pending = []


def wait_all(copies):
    for c in copies:
        c.wait_recv()


class Weights:
    def __init__(self, net, buf, z, x, c):
        self.net, self.buf, self.z, self.x, self.c = net, buf, z, x, c
        self.across = {}

    def first(self):
        net, buf, z, x, c = self.net, self.buf, self.z, self.x, self.c
        a = buf.at[z, x, c, :, pl.ds(0, 768)]
        b = buf.at[z, x, c, :, pl.ds(768, 768)]
        self.a1 = [net.copy(a, a, x=lax.rem(x + d, NX)) for d in (1, 3, 2)]
        self.b1 = [net.copy(b, b, z=lax.rem(z + d, NZ)) for d in (1, 7, 2, 6, 3, 5, 4)]

    def plane(self, k):
        return lax.rem(self.z + k + NZ, NZ)

    def share_plane(self, k):
        part = self.buf.at[self.plane(k), :, self.c, :, pl.ds(0, 768)]
        self.across["a", k] = self.net.copy(part, part, c=1 - self.c)

    def share_set(self, k):
        part = self.buf.at[:, lax.rem(self.x + k + NX, NX), self.c, :, pl.ds(768, 768)]
        self.across["b", k] = self.net.copy(part, part, c=1 - self.c)

    def z_step(self, k):
        net, buf, z, c = self.net, self.buf, self.z, self.c
        xs = (pl.ds(0, NX), pl.ds(0, NX)) if k < 4 else (pl.ds(0, 2), pl.ds(2, 2))
        up = buf.at[self.plane(1 - k), xs[0], c, :, pl.ds(0, 768)]
        down = buf.at[self.plane(k - 1), xs[1], c, :, pl.ds(0, 768)]
        self.az = [
            net.copy(up, up, z=lax.rem(z + 1, NZ)),
            net.copy(down, down, z=lax.rem(z + NZ - 1, NZ)),
        ]

    def x_step(self, k):
        net, buf, x, c = self.net, self.buf, self.x, self.c
        zs = (pl.ds(0, NZ), pl.ds(0, NZ)) if k < 2 else (pl.ds(0, 4), pl.ds(4, 4))
        up = buf.at[zs[0], lax.rem(x + NX + 1 - k, NX), c, :, pl.ds(768, 768)]
        down = buf.at[zs[1], lax.rem(x + k - 1, NX), c, :, pl.ds(768, 768)]
        self.bx = [
            net.copy(up, up, x=lax.rem(x + 1, NX)),
            net.copy(down, down, x=lax.rem(x + NX - 1, NX)),
        ]

    def a_start(self):
        wait_all(self.a1)
        self.z_step(1)
        self.share_plane(0)

    def b_start(self):
        wait_all(self.b1)
        self.x_step(1)
        self.share_set(0)

    def a_next(self, k):
        wait_all(self.az)
        if k < 4:
            self.z_step(k + 1)
            self.share_plane(-k)
            self.share_plane(k)
        else:
            self.share_plane(4)

    def b_next(self, k):
        wait_all(self.bx)
        if k < 2:
            self.x_step(k + 1)
            self.share_set(-1)
            self.share_set(1)
        else:
            self.share_set(2)

    def have(self, *names):
        for n in names:
            self.across.pop(n).wait_recv()


def enter(z, x, c, t):
    sp = (z * NX + x) * NC + c
    n = NZ * NX * NC
    places = [{"tp": lax.rem(t + d, NT)} for d in range(1, NT)]
    places += [{"x": lax.rem(x + d, NX)} for d in range(1, NX)]
    places += [{"z": lax.rem(z + d, NZ)} for d in range(1, NZ)]
    places += [{"c": 1 - c}]
    for d in (1, n - 1):
        places += [{**span_at(lax.rem(sp + d, n)), "tp": k} for k in range(NT)]
    barrier = pltpu.get_barrier_semaphore()
    for place in places:
        pl.semaphore_signal(barrier, inc=1, device_id=place, device_id_type=MESH)
    pl.semaphore_wait(barrier, len(places))


def span_at(sp):
    return {"z": sp // (NX * NC), "x": lax.rem(sp // NC, NX), "c": lax.rem(sp, NC)}


def multiply(rows, planes, buf, acc, base, width, first):
    def body(n, carry):
        cols = pl.ds(pl.multiple_of(base + n * 256, 256), 256)
        for i, k in enumerate(planes):
            w = buf[k, :, :, :, cols].reshape(NX * NC * 32, 256)
            part = jnp.dot(rows[k], w, preferred_element_type=f32)
            if first and i == 0:
                acc[:, cols] = part
            else:
                acc[:, cols] += part
        return carry

    lax.fori_loop(0, width // 256, body, 0)


def gather_inputs_start(net, x_hbm, x_own, X, XH, G, gain, z, x, c, t):
    sp = (z * NX + x) * NC + c
    after = span_at(lax.rem(sp + 1, NZ * NX * NC))
    x_own.wait()
    up, down = lax.rem(t + 1, NT), lax.rem(t + NT - 1, NT)
    own = X.at[t]
    half = TOK // 2
    top, low = own.at[pl.ds(0, half)], own.at[pl.ds(half, half)]
    g = [net.copy(gain, G.at[t], tp=lax.rem(t + d, NT)) for d in range(1, NT)]
    ys = {}
    ys["u0"] = net.copy(top, top, tp=up)
    ys["d1"] = net.copy(low, low, tp=down)
    ys["u1"] = net.copy(low, low, tp=up)
    ys["d0"] = net.copy(top, top, tp=down)
    last = own.at[pl.ds(TOK - HALO, HALO)]
    h = [net.copy(last, XH.at[t], **after, tp=lax.rem(t + d, NT)) for d in range(NT)]
    return g, ys, h


def gather_inputs_forward(net, ys, X, t):
    up, down = lax.rem(t + 1, NT), lax.rem(t + NT - 1, NT)
    half = TOK // 2
    ys["u0"].wait_recv()
    low_src = X.at[down].at[pl.ds(0, half)]
    ys["f0"] = net.copy(low_src, low_src, tp=up)
    ys["d1"].wait_recv()
    high_src = X.at[up].at[pl.ds(half, half)]
    ys["f1"] = net.copy(high_src, high_src, tp=down)


def scale_block(b, X, G, N, SQ, first):
    def body(i, carry):
        r = pl.ds(pl.multiple_of(i * 128, 128), 128)
        ro = pl.ds(pl.multiple_of(i * 128 + HALO, 32), 128)
        v = X[b, r, :].astype(f32)
        n = (v * G[b, 0:1, :]).astype(bf16)
        N[2 * b, ro, :] = n[:, :256]
        N[2 * b + 1, ro, :] = n[:, 256:]
        s = v * v
        s = s[:, 0:128] + s[:, 128:256] + s[:, 256:384] + s[:, 384:512]
        SQ[ro, :] = s if first else SQ[ro, :] + s
        return carry

    lax.fori_loop(0, TOK // 128, body, 0)


def scale_halo(XH, G, N, SQ, sp):
    total = None
    for b in range(NT):
        v = jnp.where(sp > 0, XH[b].astype(f32), 0.0)
        n = (v * G[b, 0:1, :]).astype(bf16)
        N[2 * b, 0:HALO, :] = n[:, :256]
        N[2 * b + 1, 0:HALO, :] = n[:, 256:]
        s = v * v
        s = s[:, 0:128] + s[:, 128:256] + s[:, 256:384] + s[:, 384:512]
        total = s if total is None else total + s
    SQ[0:HALO, :] = total
highest = lax.Precision.HIGHEST


def gather_and_project(
    x_hbm, gain, wq, wk, wv, wo, wp, wout, ig, fg,
    qkv_out, gate_out, keep_out, og_out, wout_out,
    X, XH, G, N, SQ, INV, W1, W2, A1, A2, send_sems, recv_sems, local_sems,
):
    z, x, c, t = (lax.axis_index(n) for n in SP_TP)
    sp = (z * NX + x) * NC + c
    net = Ring(send_sems, recv_sems, local_sems)
    x_own = net.local(x_hbm, X.at[t])
    mine1, mine2 = W1.at[z, x, c], W2.at[z, x, c]
    load1 = [net.local(w, mine1.at[:, pl.ds(512 * i, 512)]) for i, w in enumerate((wq, wk, wv))]
    load2 = [
        net.local(wo, mine2.at[:, pl.ds(0, 512)]),
        net.local(wp, mine2.at[:, pl.ds(512, 256)]),
        net.local(wout, mine2.at[:, pl.ds(768, 768)]),
    ]
    enter(z, x, c, t)
    for l in load1:
        l.wait()
    w1 = Weights(net, W1, z, x, c)
    w2 = Weights(net, W2, z, x, c)
    w1.first()
    g, ys, h = gather_inputs_start(net, x_hbm, x_own, X, XH, G, gain, z, x, c, t)
    G[t] = gain[...]
    scale_block(t, X, G, N, SQ, True)
    w1.a_start()
    gather_inputs_forward(net, ys, X, t)
    w1.b_start()
    for l in load2:
        l.wait()
    w1.a_next(1)
    w2.first()
    wait_all(g)
    ys["u1"].wait_recv()
    ys["d0"].wait_recv()
    scale_block(lax.rem(t + NT - 1, NT), X, G, N, SQ, False)
    w1.b_next(1)
    scale_block(lax.rem(t + 1, NT), X, G, N, SQ, False)
    w1.a_next(2)
    w2.a_start()
    w2.b_start()
    ys["f0"].wait_recv()
    ys["f1"].wait_recv()
    scale_block(lax.rem(t + 2, NT), X, G, N, SQ, False)
    wait_all(h)
    scale_halo(XH, G, N, SQ, sp)
    INV[...] = lax.rsqrt(jnp.sum(SQ[...], axis=1, keepdims=True) / (NT * 512) + epsilon)
    gates = jnp.zeros((TOK, 8), f32)
    keeps = jnp.zeros((TOK, 8), f32)
    for k in range(NZ):
        rows = N[k, HALO:, :]
        gates += jnp.dot(rows, ig[k * 256 : (k + 1) * 256, :], preferred_element_type=f32)
        keeps += jnp.dot(rows, fg[k * 256 : (k + 1) * 256, :], preferred_element_type=f32)
    gate_out[...] = gates * INV[HALO:, :]
    keep_out[...] = keeps * INV[HALO:, :]
    w1.a_next(3)
    w1.b_next(2)
    w1.have(("a", 0), ("a", -1), ("a", 1), ("a", -2), ("a", 2))
    w2.a_next(1)
    multiply(N, [w1.plane(k) for k in (0, -1, 1, -2, 2)], W1, A1, 0, 768, True)
    w1.a_next(4)
    w2.b_next(1)
    w1.have(("a", -3), ("a", 3))
    multiply(N, [w1.plane(k) for k in (-3, 3)], W1, A1, 0, 768, False)
    w1.have(("b", 0), ("b", -1), ("b", 1), ("b", 2))
    multiply(N, list(range(NZ)), W1, A1, 768, 768, True)
    w1.have(("a", 4))
    multiply(N, [w1.plane(4)], W1, A1, 0, 768, False)
    qkv_out[...] = (A1[...] * INV[...]).astype(bf16)
    w2.a_next(2)
    w2.b_next(2)
    w2.a_next(3)
    w2.a_next(4)
    w2.have(*[("a", k) for k in (0, -1, 1, -2, 2, -3, 3, 4)])
    multiply(N, list(range(NZ)), W2, A2, 0, 768, True)
    og_out[...] = (A2[...] * INV[...]).astype(bf16)
    w2.have(*[("b", k) for k in (0, -1, 1, 2)])
    wout_out[...] = W2[:, :, :, :, 768:].reshape(2048, 768)
    net.drain()


def projections(inputs, gain, weights, wout, ig, fg):
    hbm = pl.BlockSpec(memory_space=pl.ANY)
    vmem = pl.BlockSpec(memory_space=pltpu.VMEM)
    return pl.pallas_call(
        gather_and_project,
        out_shape=(
            jax.ShapeDtypeStruct((ROWS, 1536), bf16),
            jax.ShapeDtypeStruct((TOK, 8), f32),
            jax.ShapeDtypeStruct((TOK, 8), f32),
            jax.ShapeDtypeStruct((ROWS, 768), bf16),
            jax.ShapeDtypeStruct((2048, 768), bf16),
        ),
        in_specs=[hbm, vmem] + [hbm] * 6 + [vmem] * 2,
        out_specs=(vmem,) * 5,
        scratch_shapes=[
            pltpu.VMEM((NT, TOK, 512), bf16),
            pltpu.VMEM((NT, HALO, 512), bf16),
            pltpu.VMEM((NT, 8, 512), f32),
            pltpu.VMEM((NZ, ROWS, 256), bf16),
            pltpu.VMEM((ROWS, 128), f32),
            pltpu.VMEM((ROWS, 1), f32),
            pltpu.VMEM((NZ, NX, NC, 32, 1536), bf16),
            pltpu.VMEM((NZ, NX, NC, 32, 1536), bf16),
            pltpu.VMEM((ROWS, 1536), f32),
            pltpu.VMEM((ROWS, 768), f32),
            pltpu.SemaphoreType.DMA((96,)),
            pltpu.SemaphoreType.DMA((96,)),
            pltpu.SemaphoreType.DMA((8,)),
        ],
        compiler_params=pltpu.CompilerParams(
            collective_id=0, has_side_effects=True, vmem_limit_bytes=60 * 2**20
        ),
        name="gather_and_project",
    )(inputs, gain, *weights, wout, ig, fg)


def copy_for_each(array, axis):
    copies = jnp.broadcast_to(array, (lax.axis_size(axis), *array.shape))
    return lax.all_to_all(copies, axis, split_axis=0, concat_axis=0, tiled=True)


def taken_together(array, axis):
    everything = copy_for_each(array, axis)
    return jnp.sum(everything, axis=0)


def joined_along(pieces, dim):
    dims = list(pieces.shape[1:])
    dims[dim] *= pieces.shape[0]
    return jnp.moveaxis(pieces, 0, dim).reshape(dims)


def gather_directly(array, axis, dim):
    pieces = copy_for_each(array, axis)
    return joined_along(pieces, dim)


def in_one_piece(arrays, axis, dim, along):
    both = jnp.concatenate(arrays, axis=along)
    result, at, done = (lax.all_gather(both, axis, axis=dim, tiled=True), 0, [])
    for a in arrays:
        done.append(lax.slice_in_dim(result, at, at + a.shape[along], axis=along))
        at += a.shape[along]
    return tuple(done)


def shifted(block, axis, distance):
    devices = range(lax.axis_size(axis))
    route = [(i - distance, i) for i in devices if i - distance in devices]
    return lax.ppermute(block, axis, route)


def nothing_yet(array, identity):
    return jax.tree.map(
        lambda part, zero: jnp.zeros_like(part) + jnp.asarray(zero, part.dtype), array, identity
    )


def collected_together(array, axis):
    leaves = jax.tree.leaves(array)
    turns = sorted(range(len(leaves)), key=lambda k: -leaves[k].size)
    width = (1, *leaves[turns[0]].shape)[-1]
    lines = [
        jnp.pad(leaves[k].reshape(-1), (0, -leaves[k].size % width)).reshape(-1, width)
        for k in turns
    ]
    both, at, found = (lax.all_gather(jnp.concatenate(lines), axis), 0, {})
    for k, line in zip(turns, lines):
        slab = both[:, at : at + len(line)].reshape(len(both), -1)
        found[k] = slab[:, : leaves[k].size].reshape(-1, *leaves[k].shape)
        at += len(line)
    numbers = iter(range(len(leaves)))
    return jax.tree.map(lambda _: found[next(numbers)], array)


def carried_in(array, axes, combine, identity):
    before = start = nothing_yet(array, identity)
    subtotal = array
    for axis in reversed(axes):
        count, place = (lax.axis_size(axis), lax.axis_index(axis))
        pieces = collected_together(subtotal, axis)
        inside, subtotal = (start, start)
        for k in range(count):
            passed = k < place
            subtotal = combine(subtotal, jax.tree.map(lambda part: part[k], pieces))
            inside = jax.tree.map(lambda new, old: jnp.where(passed, new, old), subtotal, inside)
        before = combine(inside, before)
    return before


def rows_first(arrays, axis, dims):
    turned = [jnp.moveaxis(a, dim, 0) for a, dim in zip(arrays, dims)]
    both = jnp.concatenate([t.reshape(len(t), -1) for t in turned], axis=1)
    result, at, done = (lax.all_gather(both, axis, axis=0, tiled=True), 0, [])
    for t, dim in zip(turned, dims):
        slab = result[:, at : at + t[0].size].reshape(-1, *t.shape[1:])
        done.append(jnp.moveaxis(slab, 0, dim))
        at += t[0].size
    return tuple(done)


def cut_along(array, dim, count):
    dims = array.shape
    pieces = array.reshape(*dims[:dim], count, dims[dim] // count, *dims[dim + 1 :])
    return jnp.moveaxis(pieces, dim, 0)


def summed_on_arrival(array, axis, dim):
    count = lax.axis_size(axis)
    pieces = lax.all_to_all(cut_along(array, dim, count), axis, 0, 0, tiled=True)
    return jnp.sum(pieces.astype(jnp.float32), axis=0)


def causal_taps(padded, taps):
    span_rows = padded.shape[0] - taps.shape[0] + 1
    running = jnp.zeros((span_rows, padded.shape[1]), jnp.float32)
    for lag_index in range(taps.shape[0]):
        running = running + taps[lag_index] * padded[lag_index : lag_index + span_rows].astype(
            jnp.float32
        )
    return running


def combine_states(earlier, later):
    memory_early, normal_early, ceiling_early, fall_early = earlier
    memory_late, normal_late, ceiling_late, fall_late = later
    ceiling = jnp.maximum(fall_late + ceiling_early, ceiling_late)
    left_weight = jnp.exp(fall_late + ceiling_early - ceiling)
    right_weight = jnp.exp(ceiling_late - ceiling)
    memory = left_weight[:, None, None] * memory_early + right_weight[:, None, None] * memory_late
    normal = left_weight[:, None] * normal_early + right_weight[:, None] * normal_late
    return (memory, normal, ceiling, fall_early + fall_late)


def cell_outputs(queries, key_rows, value_rows, log_in, cumulative, memory, normalizer, stabilizer):
    length = queries.shape[0]
    query_wide = queries.astype(jnp.float32)
    cum_heads = cumulative.T
    in_heads = log_in.T
    causal = jnp.arange(length)[:, None] >= jnp.arange(length)[None, :]
    decay_log = cum_heads[:, :, None] - cum_heads[:, None, :] + in_heads[:, None, :]
    decay_log = jnp.where(causal[None, :, :], decay_log, -jnp.inf)
    carried_log = cum_heads + stabilizer[:, None]
    ceiling = jnp.maximum(carried_log, jnp.max(decay_log, axis=2))
    within = jnp.exp(decay_log - ceiling[:, :, None])
    carried = jnp.exp(carried_log - ceiling)
    raw_scores = jnp.einsum("thd,shd->hts", queries, key_rows, preferred_element_type=jnp.float32)
    scores = (raw_scores * within).astype(jnp.bfloat16)
    numerator = carried.T[:, :, None] * jnp.einsum(
        "hvk,thk->thv", memory, query_wide, precision=highest
    )
    numerator = numerator + jnp.einsum(
        "hts,shv->thv", scores, value_rows, preferred_element_type=jnp.float32
    )
    denominator = (
        carried.T * jnp.einsum("hk,thk->th", normalizer, query_wide, precision=highest)
        + jnp.sum(scores.astype(jnp.float32), axis=2).T
    )
    return numerator / jnp.maximum(jnp.abs(denominator), jnp.exp(-ceiling.T))[:, :, None]


def local(
    inputs,
    norm_gain,
    query_weight,
    key_weight,
    value_weight,
    outgate_weight,
    inputgate_weight,
    forget_weight,
    forget_bias,
    conv_query,
    conv_key,
    cell_gain,
    pool_weight,
    group_weight,
    pool_gain,
    cell_out_weight,
    pool_out_weight,
):
    gain = jnp.broadcast_to(norm_gain.astype(f32)[None, :], (8, 512))
    wout = jnp.concatenate([cell_out_weight, pool_out_weight], axis=0).T
    qkv, log_in_all, keep_all, ogp, wout_all = projections(
        inputs,
        gain,
        (query_weight, key_weight, value_weight, outgate_weight, pool_weight),
        wout,
        inputgate_weight,
        forget_weight,
    )
    tp_index = lax.axis_index("tp")
    sp_index = lax.axis_index(SP)
    tokens_here = inputs.shape[0]
    sequence_log = math.log(tokens_here * lax.axis_size(SP))
    local_heads = forget_bias.shape[0]
    log_in = lax.dynamic_slice_in_dim(log_in_all, tp_index * local_heads, local_heads, 1)
    log_keep = jax.nn.log_sigmoid(
        lax.dynamic_slice_in_dim(keep_all, tp_index * local_heads, local_heads, 1)
        + forget_bias
        + sequence_log
    )
    widest = 2**LEVELS - 1
    query_width = 512
    before = jnp.concatenate([qkv[HALO - widest : HALO, :1024], ogp[HALO - widest : HALO, 512:]], axis=1)
    query_pre, key_pre, value_rows = (qkv[HALO:, 512 * i : 512 * (i + 1)] for i in range(3))
    outgate_pre, pool_pre = ogp[HALO:, :512], ogp[HALO:, 512:]
    margin = conv_query.shape[0] - 1
    query_taps = causal_taps(
        jnp.concatenate([before[widest - margin :, :query_width], query_pre], axis=0), conv_query
    )
    key_taps = causal_taps(
        jnp.concatenate(
            [before[widest - margin :, query_width : 2 * query_width], key_pre], axis=0
        ),
        conv_key,
    )
    pool_before = before[:, 2 * query_width :]
    head_size = query_width // local_heads
    queries = (
        (jax.nn.silu(query_taps) * head_size ** (-0.5))
        .astype(jnp.bfloat16)
        .reshape(tokens_here, local_heads, head_size)
    )
    key_rows = (
        jax.nn.silu(key_taps).astype(jnp.bfloat16).reshape(tokens_here, local_heads, head_size)
    )
    value_heads = value_rows.reshape(tokens_here, local_heads, head_size)
    key_wide = key_rows.astype(jnp.float32)
    cumulative = jnp.cumsum(log_keep, axis=0)
    final_log = cumulative[-1]
    lead_log = final_log[None, :] - cumulative + log_in
    own_ceiling = jnp.max(lead_log, axis=0)
    share_weight = jnp.exp(lead_log - own_ceiling[None, :])
    weighted = (value_heads.astype(jnp.float32) * share_weight[:, :, None]).astype(jnp.bfloat16)
    own_memory = jnp.einsum("shv,shk->hvk", weighted, key_rows, preferred_element_type=jnp.float32)
    own_normalizer = jnp.einsum("sh,shk->hk", share_weight, key_wide, precision=highest)
    identity = (
        jnp.zeros_like(own_memory),
        jnp.zeros_like(own_normalizer),
        jnp.full_like(own_ceiling, big_negative),
        jnp.zeros_like(final_log),
    )
    memory_in, normalizer_in, ceiling_in, fall_in = carried_in(
        (own_memory, own_normalizer, own_ceiling, final_log), SP, combine_states, identity
    )
    hidden = cell_outputs(
        queries, key_rows, value_heads, log_in, cumulative, memory_in, normalizer_in, ceiling_in
    )
    normalized = hidden * lax.rsqrt(jnp.mean(hidden * hidden, axis=2, keepdims=True) + epsilon)
    cell_mix = (
        normalized.reshape(tokens_here, query_width)
        * cell_gain
        * jax.nn.sigmoid(outgate_pre.astype(jnp.float32))
    ).astype(jnp.bfloat16)
    local_groups = group_weight.shape[0]
    group_width = pool_pre.shape[1] // local_groups
    group_ids = tp_index * local_groups + jnp.arange(local_groups, dtype=jnp.int32)
    reach_rows = 2 ** (1 + group_ids % LEVELS)
    row_ids = jnp.arange(tokens_here, dtype=jnp.int32)
    column_ids = jnp.arange(tokens_here + widest, dtype=jnp.int32)
    distance = row_ids[:, None] + widest - column_ids[None, :]
    band = (
        (distance[None, :, :] >= 0) & (distance[None, :, :] < reach_rows[:, None, None])
    ).astype(jnp.bfloat16)
    extended = jnp.concatenate([pool_before, pool_pre], axis=0).reshape(
        tokens_here + widest, local_groups, group_width
    )
    window_sum = jnp.einsum("gts,sgc->tgc", band, extended, preferred_element_type=jnp.float32)
    global_rows = sp_index * tokens_here + row_ids
    counted = jnp.minimum(global_rows[:, None] + 1, reach_rows[None, :]).astype(jnp.float32)
    own_rows = pool_pre.reshape(tokens_here, local_groups, group_width).astype(jnp.float32)
    pooled = (window_sum / counted[:, :, None] - own_rows).astype(jnp.bfloat16)
    grouped_out = jnp.einsum(
        "tgc,gcd->tgd", pooled, group_weight, preferred_element_type=jnp.float32
    )
    pool_mix = (grouped_out.reshape(tokens_here, local_groups * group_width) * pool_gain).astype(
        jnp.bfloat16
    )
    mixed = summed_on_arrival(
        lax.dot_general(
            jnp.concatenate([cell_mix, pool_mix], axis=1),
            wout_all,
            (((1,), (1,)), ((), ())),
            preferred_element_type=jnp.float32,
        ).astype(jnp.bfloat16),
        "tp",
        0,
    )
    return mixed.astype(jnp.bfloat16)


def solution(mesh):
    split = Mesh(mesh.devices.reshape(8, 4, 2, mesh.shape["tp"]), SP_TP)
    return jax.shard_map(
        local,
        mesh=split,
        in_specs=(
            P(SP, "tp"),
            P("tp"),
            P(SP, "tp"),
            P(SP, "tp"),
            P(SP, "tp"),
            P(SP, "tp"),
            P(),
            P(),
            P("tp"),
            P(None, "tp"),
            P(None, "tp"),
            P("tp"),
            P(SP, "tp"),
            P("tp", None, None),
            P("tp"),
            P("tp", SP),
            P("tp", SP),
        ),
        out_specs=P(SP_TP, None),
        check_vma=False,
    )
```
